32 devices in a mesh: kv: 8 (over z, y), tp: 4 (over x, core).
Axes of the slice: x: 2, y: 2, z: 4, core: 2. Of those that a mesh axis runs over, the one named last changes fastest.
Arguments:
- tokens: bfloat16 [64, 4096], P(None, 'kv'), may hold values from -170 to 170
- mix_gain: float32 [4096], P('kv'), may hold values from 0.1 to 1.9
- w_query: bfloat16 [4096, 2048], P('kv', 'tp'), may hold values from -0.09375 to 0.09375
- w_key: bfloat16 [4096, 512], P('kv', 'tp'), may hold values from -0.09375 to 0.09375
- w_value: bfloat16 [4096, 512], P('kv', 'tp'), may hold values from -0.09375 to 0.09375
- w_forget: bfloat16 [4096, 32], P('kv', 'tp'), may hold values from -0.09375 to 0.09375
- query_gain: float32 [64], replicated, may hold values from 0.1 to 1.9
- key_cache: bfloat16 [64, 8, 64, 8192], P(None, 'tp', None, 'kv'), may hold values from -1300 to 1300
- value_cache: bfloat16 [64, 8, 64, 8192], P(None, 'tp', None, 'kv'), may hold values from -8 to 8
- decay_cache: float32 [64, 32, 8192], P(None, 'tp', 'kv'), may hold values from -1066.96 to 0, as said below
- w_out: bfloat16 [2048, 4096], P('tp', 'kv'), may hold values from -1 to 1
- mlp_gain: float32 [4096], P('kv'), may hold values from 0.1 to 1.9
- w_up: bfloat16 [4096, 16384], P('kv', 'tp'), may hold values from -0.09375 to 0.09375
- w_down: bfloat16 [16384, 4096], P('tp', 'kv'), may hold values from -0.046875 to 0.046875
Outputs:
- layer_out: bfloat16 [64, 4096], P(None, 'kv')
The draws below stay inside these ranges and needn't reach their ends.
Inputs may be any that keep to these rules, and one draw needn't show every extreme that they name: `decay_cache`: each entry is the sum of the non-positive log forget gates of the later cached positions of its sequence and head: 0 at the last cached position, never smaller at a later position.
All inputs are finite; a program needn't handle non-finite values.
Results may differ from the reference program's by a relative error of at most 0.015.
Values may be sent and summed in bfloat16 or wider, within the bound.
A program may use at most 128 MiB of HBM per device.

```python
import jax
import jax.numpy as jnp
from jax import lax

D = 4096
HEADS = 32
KV_HEADS = 8
HEAD_DIM = 64
FF = 16384
BATCH = 64
POSITIONS_LOCAL = 1024
POSITIONS = 8192
HEAD_GROUP = 8
FF_GROUP = 4096


def draw_tokens(key, part):
    keys = jax.random.split(key, 2)
    columns = jnp.arange(D, dtype=jnp.float32) / D
    base = jnp.clip(jax.random.normal(keys[0], (BATCH, D), jnp.float32), -4.0, 4.0)
    row_scale = jnp.exp(jax.random.uniform(keys[1], (BATCH, 1), jnp.float32, 0.0, jnp.log(3.0)))
    rising = 3.0 ** columns
    return (base * row_scale * rising[None, :]).astype(jnp.bfloat16)


def draw_key_cache(key, part):
    keys = jax.random.split(key, 3)
    base = jnp.clip(jax.random.normal(keys[0], (BATCH, KV_HEADS, HEAD_DIM, POSITIONS), jnp.float32), -5.0, 5.0)
    low_strength = jnp.log(40.0)
    high_strength = jnp.log(200.0)
    strength = jnp.exp(jax.random.uniform(keys[1], (BATCH, KV_HEADS, 1, 1), jnp.float32, low_strength, high_strength))
    spot = jax.random.randint(keys[2], (BATCH, KV_HEADS, 1, 1), 0, POSITIONS - 1)
    current_location = jnp.arange(POSITIONS).reshape(1, 1, 1, POSITIONS)
    anchor = jnp.take_along_axis(base, jnp.broadcast_to(spot, (BATCH, KV_HEADS, HEAD_DIM, 1)), axis=3)
    bump = jnp.where(current_location == spot + 1, 1.01, 1.0)
    planted = (current_location == spot) | (current_location == spot + 1)
    base = jnp.where(planted, anchor * strength * bump, base)
    return base.astype(jnp.bfloat16)


def draw_value_cache(key, part):
    keys = jax.random.split(key, 2)
    blocks = POSITIONS // POSITIONS_LOCAL
    base = jnp.clip(jax.random.normal(keys[0], (BATCH, KV_HEADS, HEAD_DIM, POSITIONS), jnp.float32), -5.0, 5.0)
    means = jnp.clip(jax.random.normal(keys[1], (BATCH, KV_HEADS, HEAD_DIM, blocks), jnp.float32), -3.0, 3.0)
    return (base + jnp.repeat(means, POSITIONS_LOCAL, axis=3)).astype(jnp.bfloat16)


def draw_decay_cache(key, part):
    keys = jax.random.split(key, 7)
    fast_share = 0.5
    is_fast = jax.random.uniform(keys[0], (BATCH, HEADS, 1), jnp.float32) < fast_share
    slow_rate = jax.random.uniform(keys[1], (BATCH, HEADS, 1), jnp.float32, 0.3, 0.8) / POSITIONS
    fast_rate = jnp.exp(jax.random.uniform(keys[2], (BATCH, HEADS, 1), jnp.float32, jnp.log(0.01), jnp.log(0.04)))
    baseline_rate = jnp.where(is_fast, fast_rate, slow_rate)
    blocks = POSITIONS // POSITIONS_LOCAL
    block_multiplier = jnp.exp(jax.random.uniform(keys[3], (BATCH, HEADS, blocks), jnp.float32, jnp.log(0.5), jnp.log(2.0)))
    coarse_estimate = jax.random.uniform(keys[4], (BATCH, HEADS, POSITIONS), jnp.float32, 0.5, 1.5)
    chosen_places = jax.random.randint(keys[5], (BATCH, HEADS, 2), 0, POSITIONS)
    loss_values = jax.random.uniform(keys[6], (BATCH, HEADS, 2), jnp.float32, 0.22, 0.69)
    current_location = jnp.arange(POSITIONS).reshape(1, 1, POSITIONS)
    sudden_jump = jnp.where(current_location == chosen_places[:, :, 0:1], loss_values[:, :, 0:1], 0.0)
    sudden_jump = sudden_jump + jnp.where(current_location == chosen_places[:, :, 1:2], loss_values[:, :, 1:2], 0.0)
    per_step_rate = baseline_rate * jnp.repeat(block_multiplier, POSITIONS_LOCAL, axis=2) * coarse_estimate + sudden_jump
    after = jnp.flip(jnp.cumsum(jnp.flip(per_step_rate, axis=2), axis=2), axis=2) - per_step_rate
    return -after


def shard_levels(key, extent, cuts, low, high):
    def one(axis_at, blocks):
        draws = jax.random.uniform(jax.random.fold_in(jax.random.fold_in(key, 6), axis_at), (blocks,), jnp.float32, low / len(cuts), high / len(cuts))
        return jnp.repeat(jnp.exp(draws), extent[axis_at] // blocks).reshape((-1,) + (1,) * (len(extent) - axis_at - 1))

    level = one(*cuts[0])
    for cut in cuts[1:]:
        level = level * one(*cut)
    return level


def bell_draw(own_key, dims, scale, limit, shards=(), kind=jnp.bfloat16):
    entries = jax.random.normal(own_key, dims, jnp.float32) * scale
    if len(shards) > 0:
        entries = shard_levels(own_key, dims, shards, -0.22, 0.18) * entries
    return jnp.clip(entries, min=-limit, max=limit).astype(kind)


def setup_inputs(seed: int = 0) -> dict:
    arg_keys = jax.random.split(jax.random.key(seed), 15)
    return {
        "tokens": draw_tokens(jax.random.fold_in(arg_keys[14], 71), 0),
        "mix_gain": jnp.clip(1.0 + 0.18 * jax.random.normal(arg_keys[1], (D,), jnp.float32), 0.1, 1.9),
        "w_query": bell_draw(arg_keys[2], (D, HEADS * HEAD_DIM), D ** -0.5, 0.09375, ((0, 8), (1, 4))),
        "w_key": bell_draw(arg_keys[3], (D, KV_HEADS * HEAD_DIM), D ** -0.5, 0.09375, ((0, 8), (1, 4))),
        "w_value": bell_draw(arg_keys[4], (D, KV_HEADS * HEAD_DIM), D ** -0.5, 0.09375, ((0, 8), (1, 4))),
        "w_forget": bell_draw(arg_keys[5], (D, HEADS), D ** -0.5, 0.09375, ((0, 8), (1, 4))),
        "query_gain": jnp.clip(1.0 + 0.18 * jax.random.normal(arg_keys[6], (HEAD_DIM,), jnp.float32), 0.1, 1.9),
        "key_cache": draw_key_cache(jax.random.fold_in(arg_keys[14], 71), 0),
        "value_cache": draw_value_cache(jax.random.fold_in(arg_keys[14], 71), 0),
        "decay_cache": draw_decay_cache(jax.random.fold_in(arg_keys[14], 71), 0),
        "w_out": bell_draw(arg_keys[10], (HEADS * HEAD_DIM, D), (HEADS * HEAD_DIM // 64) ** -0.5, 1.0, ((0, 4), (1, 8))),
        "mlp_gain": jnp.clip(1.0 + 0.18 * jax.random.normal(arg_keys[11], (D,), jnp.float32), 0.1, 1.9),
        "w_up": bell_draw(arg_keys[12], (D, FF), D ** -0.5, 0.09375, ((0, 8), (1, 4))),
        "w_down": bell_draw(arg_keys[13], (FF, D), FF ** -0.5, 0.046875, ((0, 4), (1, 8))),
    }


EPS = 1e-06

def rounded(value):
    return lax.optimization_barrier(value.astype(jnp.bfloat16)).astype(jnp.float32)

def attend_one(operands):
    query_row, keys_row, values_row, decay_row, forget_row, key_row, value_row = operands
    score_scale = HEAD_DIM ** (-0.5)
    scores = jnp.einsum('gjd,gdp->gjp', query_row.astype(jnp.float32), keys_row.astype(jnp.float32)) * score_scale
    scores = scores + decay_row + forget_row[..., None]
    own_score = jnp.einsum('gjd,gd->gj', query_row.astype(jnp.float32), key_row.astype(jnp.float32)) * score_scale
    peak_score = jnp.maximum(lax.optimization_barrier(jnp.max(scores, axis=-1)), own_score)
    weights = jnp.exp(scores - peak_score[..., None])
    own_weight = jnp.exp(own_score - peak_score)
    totals = lax.optimization_barrier(jnp.sum(weights, axis=-1)) + own_weight
    summed = jnp.einsum('gjp,gdp->gjd', rounded(weights), values_row.astype(jnp.float32))
    summed = summed + rounded(own_weight)[..., None] * value_row.astype(jnp.float32)[:, None, :]
    return summed / totals[..., None]

def reference(tokens, mix_gain, w_query, w_key, w_value, w_forget, query_gain, key_cache, value_cache, decay_cache, w_out, mlp_gain, w_up, w_down):
    stream = tokens.astype(jnp.float32)
    scale_mix = lax.rsqrt(lax.optimization_barrier(jnp.mean(stream * stream, axis=1, keepdims=True)) + EPS)
    normed_mix = (stream * mix_gain.astype(jnp.float32)).astype(jnp.bfloat16)
    query_raw = scale_mix * jnp.dot(normed_mix, w_query, preferred_element_type=jnp.float32)
    key_raw = scale_mix * jnp.dot(normed_mix, w_key, preferred_element_type=jnp.float32)
    value_raw = scale_mix * jnp.dot(normed_mix, w_value, preferred_element_type=jnp.float32)
    forget_raw = scale_mix * jnp.dot(normed_mix, w_forget, preferred_element_type=jnp.float32)
    heads_raw = query_raw.reshape(BATCH, HEADS, HEAD_DIM)
    inverse = lax.rsqrt(lax.optimization_barrier(jnp.mean(heads_raw * heads_raw, axis=-1, keepdims=True)) + EPS)
    query = (heads_raw * inverse * query_gain.astype(jnp.float32)).astype(jnp.bfloat16)
    sharing = HEADS // KV_HEADS
    query = query.reshape(BATCH, KV_HEADS, sharing, HEAD_DIM)
    key_new = key_raw.reshape(BATCH, KV_HEADS, HEAD_DIM).astype(jnp.bfloat16)
    value_new = value_raw.reshape(BATCH, KV_HEADS, HEAD_DIM).astype(jnp.bfloat16)
    log_forget = jax.nn.log_sigmoid(forget_raw).reshape(BATCH, KV_HEADS, sharing)
    decay = decay_cache.reshape(BATCH, KV_HEADS, sharing, -1)
    head_output = lax.map(attend_one, (query, key_cache, value_cache, decay, log_forget, key_new, value_new))
    attended = head_output.reshape(BATCH, HEADS * HEAD_DIM).astype(jnp.bfloat16)
    group_count = HEADS // HEAD_GROUP
    head_width = HEAD_GROUP * HEAD_DIM
    partials = jnp.einsum('bgk,gkd->bgd', attended.reshape(BATCH, group_count, head_width).astype(jnp.float32), w_out.reshape(group_count, head_width, D).astype(jnp.float32))
    attn_out = lax.optimization_barrier(jnp.sum(rounded(partials), axis=1))
    residual = (stream + rounded(attn_out)).astype(jnp.bfloat16)
    residual_wide = residual.astype(jnp.float32)
    scale_mlp = lax.rsqrt(lax.optimization_barrier(jnp.mean(residual_wide * residual_wide, axis=1, keepdims=True)) + EPS)
    normed_mlp = (residual_wide * mlp_gain.astype(jnp.float32)).astype(jnp.bfloat16)
    up_proj = scale_mlp * jnp.dot(normed_mlp, w_up, preferred_element_type=jnp.float32)
    hidden = jnp.square(jax.nn.relu(up_proj)).astype(jnp.bfloat16)
    unit_groups = FF // FF_GROUP
    down_parts = jnp.einsum('bgk,gkd->bgd', hidden.reshape(BATCH, unit_groups, FF_GROUP).astype(jnp.float32), w_down.reshape(unit_groups, FF_GROUP, D).astype(jnp.float32))
    mlp_out = lax.optimization_barrier(jnp.sum(rounded(down_parts), axis=1))
    return (residual_wide + rounded(mlp_out)).astype(jnp.bfloat16)
```

```python
import functools

import jax
import jax.numpy as jnp
from jax import lax
from jax.experimental import pallas as pl
from jax.experimental.pallas import tpu as pltpu
from jax.sharding import PartitionSpec as P

MESH = pl.DeviceIdType.MESH
HEAD_DIM = 64
EPS = 1e-06
F32 = jnp.float32
BF16 = jnp.bfloat16


def greet(n, t, with_tp):
    kv, tp = lax.axis_index("kv"), lax.axis_index("tp")
    barrier = pltpu.get_barrier_semaphore()
    count = n - 1
    for i in range(1, n):
        pl.semaphore_signal(
            barrier, inc=1, device_id=(lax.rem(kv + i, n), tp), device_id_type=MESH
        )
    if with_tp:
        count += t - 1
        for i in range(1, t):
            pl.semaphore_signal(
                barrier, inc=1, device_id=(kv, lax.rem(tp + i, t)), device_id_type=MESH
            )
    pl.semaphore_wait(barrier, count)


def remote(src, dst, send, recv, kv, tp):
    return pltpu.make_async_remote_copy(
        src_ref=src,
        dst_ref=dst,
        send_sem=send,
        recv_sem=recv,
        device_id=(kv, tp),
        device_id_type=MESH,
    )


def project_kernel(
    n, t, d, tok, gain, wq, wk, wv, wf, qgain, out, parts, got, mine, ssem, rsem, asem, bsem
):
    kv, tp = lax.axis_index("kv"), lax.axis_index("tp")
    greet(n, t, False)
    rows = tok.shape[0]
    rc = rows // n
    nq, nk, nf = wq.shape[1], wk.shape[1], wf.shape[1]
    stream = tok[...].astype(F32)
    squares = jnp.sum(stream * stream, axis=1, keepdims=True)
    normed = (stream * gain[...]).astype(BF16)
    q = jnp.dot(normed, wq[...], preferred_element_type=F32)
    k = jnp.dot(normed, wk[...], preferred_element_type=F32)
    v = jnp.dot(normed, wv[...], preferred_element_type=F32)
    f = jnp.dot(normed, wf[...], preferred_element_type=F32)
    for p in range(n):
        cut = slice(p * rc, (p + 1) * rc)
        parts[p, :, 0:nq] = q[cut]
        parts[p, :, nq : nq + nk] = k[cut]
        parts[p, :, nq + nk : nq + 2 * nk] = v[cut]
        base = nq + 2 * nk
        parts[p, :, base : base + 128] = jnp.broadcast_to(squares[cut], (rc, 128))
        parts[p, :, base : base + nf] = f[cut]
    sends = []
    for i in range(1, n):
        peer = lax.rem(kv + i, n)
        c = remote(parts.at[peer], got.at[i], ssem.at[i], rsem.at[i], peer, tp)
        c.start()
        sends.append(c)
    total = parts[kv]
    for c in sends:
        c.wait_recv()
    for i in range(1, n):
        total = total + got[i]
    base = nq + 2 * nk
    scale = lax.rsqrt(total[:, base + 127 : base + 128] / d + EPS)
    scaled = total * scale
    raw = scaled[:, 0:nq]
    raw2 = raw * raw
    head = lax.broadcasted_iota(jnp.int32, raw.shape, 1) // HEAD_DIM
    inverse = jnp.zeros_like(raw)
    for h in range(nq // HEAD_DIM):
        on = head == h
        mean = jnp.sum(jnp.where(on, raw2, 0.0), axis=1, keepdims=True) / HEAD_DIM
        inverse = jnp.where(on, lax.rsqrt(mean + EPS), inverse)
    mine[:, 0:nq] = raw * inverse * qgain[...]
    mine[:, nq:base] = scaled[:, nq:base]
    gate = scaled[:, base:]
    mine[:, base:] = jnp.minimum(gate, 0.0) - jnp.log1p(jnp.exp(-jnp.abs(gate)))
    gathers = []
    for i in range(1, n):
        peer = lax.rem(kv + i, n)
        c = remote(mine, out.at[kv], asem.at[i], bsem.at[i], peer, tp)
        c.start()
        gathers.append(c)
    out[kv] = mine[...]
    for i in range(1, n):
        gathers[i - 1].wait_recv()
    for c in sends + gathers:
        c.wait_send()


def attend_kernel(sharing, q_ref, k_ref, v_ref, d_ref, o_ref):
    steps, heads, _ = q_ref.shape
    groups = heads // sharing
    row = lax.broadcasted_iota(jnp.int32, (heads, HEAD_DIM), 0) // sharing
    for i in range(steps):
        s = jnp.dot(q_ref[i], k_ref[i], preferred_element_type=F32) * (HEAD_DIM**-0.5)
        s = s + d_ref[i]
        m = jnp.max(s, axis=1, keepdims=True)
        w = jnp.exp(s - m)
        l = jnp.sum(w, axis=1, keepdims=True)
        o = lax.dot_general(
            w.astype(BF16), v_ref[i], (((1,), (1,)), ((), ())), preferred_element_type=F32
        )
        picked = o[:, 0:HEAD_DIM]
        for g in range(1, groups):
            picked = jnp.where(row == g, o[:, g * HEAD_DIM : (g + 1) * HEAD_DIM], picked)
        o_ref[i, :, 0:64] = picked
        o_ref[i, :, 64:96] = jnp.broadcast_to(m, (heads, 32))
        o_ref[i, :, 96:128] = jnp.broadcast_to(l, (heads, 32))


def rest_kernel(
    n, t, d, packed, own, tok, gain, wo_hbm, wu_hbm, wd_hbm, out,
    wo, wu, wd, got, att, allatt, full, tpa, tpb, upsend, upgot, sqs, sqgot, hid,
    wsem, sem, tsem,
):
    kv, tp = lax.axis_index("kv"), lax.axis_index("tp")
    loads = [
        pltpu.make_async_copy(a, b, wsem.at[j])
        for j, (a, b) in enumerate(((wo_hbm, wo), (wu_hbm, wu), (wd_hbm, wd)))
    ]
    for c in loads:
        c.start()
    greet(n, t, True)
    rows, heads, _ = packed.shape
    rc = rows // n
    ffc = wu.shape[1] // n
    started = []

    def send(kind, i, src, dst):
        peer = lax.rem(kv + i, n)
        c = remote(src(peer), dst, sem.at[2 * kind, i], sem.at[2 * kind + 1, i], peer, tp)
        c.start()
        started.append(c)
        return c

    def tp_sum(kind, buf, value):
        buf[tp] = value.astype(BF16)
        copies = []
        for i in range(1, t):
            c = remote(
                buf.at[tp], buf.at[tp], tsem.at[2 * kind, i], tsem.at[2 * kind + 1, i],
                kv, lax.rem(tp + i, t),
            )
            c.start()
            copies.append(c)
            started.append(c)
        for c in copies:
            c.wait_recv()
        total = buf[0].astype(F32)
        for j in range(1, t):
            total = total + buf[j].astype(F32)
        return total.astype(BF16).astype(F32)

    copies = [
        send(0, i, lambda p: packed.at[pl.ds(p * rc, rc)], got.at[i]) for i in range(1, n)
    ]
    mine = packed[pl.ds(kv * rc, rc)]
    extra = own[pl.ds(kv * rc, rc)]
    own_score = extra[:, :, 64:65]
    forget = extra[:, :, 96:97]
    for c in copies:
        c.wait_recv()
    blocks = [mine] + [got[i] for i in range(1, n)]
    peaks = [b[:, :, 64:65] + forget for b in blocks]
    peak = own_score
    for p in peaks:
        peak = jnp.maximum(peak, p)
    own_weight = jnp.exp(own_score - peak)
    mass = own_weight
    summed = own_weight.astype(BF16).astype(F32) * extra[:, :, 0:64]
    for b, p in zip(blocks, peaks):
        w = jnp.exp(p - peak)
        mass = mass + w * b[:, :, 96:97]
        summed = summed + w * b[:, :, 0:64]
    head = summed / mass
    for h in range(heads):
        att[:, h * HEAD_DIM : (h + 1) * HEAD_DIM] = head[:, h, :].astype(BF16)
    copies = [send(1, i, lambda p: att, allatt.at[kv]) for i in range(1, n)]
    allatt[kv] = att[...]
    loads[0].wait()
    for c in copies:
        c.wait_recv()
    for p in range(n):
        full[p * rc : (p + 1) * rc, :] = allatt[p].astype(F32)
    attn = jnp.dot(full[...].astype(BF16), wo[...], preferred_element_type=F32)
    attn = tp_sum(0, tpa, attn)
    residual = (tok[...].astype(F32) + attn).astype(BF16).astype(F32)
    normed = (residual * gain[...]).astype(BF16)
    loads[1].wait()
    copies = []
    for i in list(range(1, n)) + [0]:
        peer = lax.rem(kv + i, n)
        cols = pl.ds(pl.multiple_of(peer * ffc, ffc), ffc)
        part = jnp.dot(normed, wu[:, cols], preferred_element_type=F32)
        if i:
            upsend[i] = part.astype(BF16)
            copies.append(send(2, i, lambda p: upsend.at[i], upgot.at[i]))
    sqs[...] = lax.dot_general(
        jnp.ones((8, residual.shape[1]), F32),
        residual * residual,
        (((1,), (1,)), ((), ())),
        preferred_element_type=F32,
        precision=lax.Precision.HIGHEST,
    )
    sq_copies = [send(3, i, lambda p: sqs, sqgot.at[i]) for i in range(1, n)]
    total = sqs[...]
    for i in range(1, n):
        sq_copies[i - 1].wait_recv()
        total = total + sqgot[i]
    r = lax.broadcasted_iota(jnp.int32, (rows, rows), 0)
    c_ = lax.broadcasted_iota(jnp.int32, (rows, rows), 1)
    wide = jnp.broadcast_to(total[0:1, :], (rows, rows))
    column = jnp.sum(jnp.where(r == c_, wide, 0.0), axis=1, keepdims=True)
    scale = lax.rsqrt(column / d + EPS)
    for i in range(1, n):
        copies[i - 1].wait_recv()
        part = part + upgot[i].astype(F32)
    hidden = jnp.square(jnp.maximum(part * scale, 0.0)).astype(BF16)
    hid[kv] = hidden
    copies = [send(4, i, lambda p: hid.at[kv], hid.at[kv]) for i in range(1, n)]
    loads[2].wait()
    here = pl.ds(pl.multiple_of(kv * ffc, ffc), ffc)
    down = jnp.dot(hidden, wd[here, :], preferred_element_type=F32)
    for i in range(1, n):
        src = lax.rem(kv + n - i, n)
        copies[i - 1].wait_recv()
        there = pl.ds(pl.multiple_of(src * ffc, ffc), ffc)
        down = down + jnp.dot(hid[src], wd[there, :], preferred_element_type=F32)
    mlp = tp_sum(1, tpb, down)
    out[...] = (residual + mlp).astype(BF16)
    for c in started:
        c.wait_send()


def shards(
    n, t, tokens, mix_gain, w_query, w_key, w_value, w_forget, query_gain,
    key_cache, value_cache, decay_cache, w_out, mlp_gain, w_up, w_down,
):
    rows, dl = tokens.shape
    d = dl * n
    rc = rows // n
    heads = w_forget.shape[1]
    groups = key_cache.shape[1]
    sharing = heads // groups
    nq, nk = w_query.shape[1], w_key.shape[1]
    span = key_cache.shape[3]
    vmem = pl.BlockSpec(memory_space=pltpu.VMEM)
    anywhere = pl.BlockSpec(memory_space=pl.ANY)
    nk_pad = nk
    width = nq + 2 * nk_pad + 128
    dma = pltpu.SemaphoreType.DMA
    proj = pl.pallas_call(
        functools.partial(project_kernel, n, t, d),
        out_shape=jax.ShapeDtypeStruct((n, rc, width), F32),
        in_specs=[vmem] * 7,
        out_specs=vmem,
        scratch_shapes=[
            pltpu.VMEM((n, rc, width), F32),
            pltpu.VMEM((n, rc, width), F32),
            pltpu.VMEM((rc, width), F32),
            dma((n,)), dma((n,)), dma((n,)), dma((n,)),
        ],
        compiler_params=pltpu.CompilerParams(collective_id=0, has_side_effects=True),
    )(
        tokens, mix_gain[None, :], w_query, w_key, w_value, w_forget,
        jnp.tile(query_gain, heads)[None, :],
    ).reshape(rows, width)
    query = proj[:, :nq].astype(BF16).reshape(rows, groups, sharing, HEAD_DIM)
    key_new = proj[:, nq : nq + nk].astype(BF16).reshape(rows, groups, HEAD_DIM)
    value_new = proj[:, nq + nk : nq + 2 * nk].astype(BF16).astype(F32)
    value_new = value_new.reshape(rows, groups, 1, HEAD_DIM)
    forget = proj[:, nq + 2 * nk : nq + 2 * nk + heads].reshape(rows, heads, 1)
    own_score = jnp.sum(
        query.astype(F32) * key_new.astype(F32)[:, :, None, :], axis=-1
    ) * (HEAD_DIM**-0.5)
    own = jnp.concatenate(
        [
            jnp.broadcast_to(value_new, (rows, groups, sharing, HEAD_DIM)).reshape(
                rows, heads, HEAD_DIM
            ),
            jnp.broadcast_to(own_score.reshape(rows, heads, 1), (rows, heads, 32)),
            jnp.broadcast_to(forget, (rows, heads, 32)),
        ],
        axis=-1,
    )
    same = jnp.eye(groups, dtype=jnp.bool_)[None, :, None, :, None]
    spread = jnp.where(same, query[:, :, :, None, :], jnp.zeros((), BF16))
    spread = spread.reshape(rows, heads, groups * HEAD_DIM)
    step = 8
    block = lambda a, b: pl.BlockSpec((step, a, b), lambda i: (i, 0, 0))
    gd = groups * HEAD_DIM
    packed = pl.pallas_call(
        functools.partial(attend_kernel, sharing),
        grid=(rows // step,),
        out_shape=jax.ShapeDtypeStruct((rows, heads, 128), F32),
        in_specs=[block(heads, gd), block(gd, span), block(gd, span), block(heads, span)],
        out_specs=block(heads, 128),
    )(
        spread,
        key_cache.reshape(rows, gd, span),
        value_cache.reshape(rows, gd, span),
        decay_cache,
    )
    ff = w_up.shape[1]
    ffc = ff // n
    return pl.pallas_call(
        functools.partial(rest_kernel, n, t, d),
        out_shape=jax.ShapeDtypeStruct((rows, dl), BF16),
        in_specs=[vmem] * 4 + [anywhere] * 3,
        out_specs=vmem,
        scratch_shapes=[
            pltpu.VMEM(w_out.shape, BF16),
            pltpu.VMEM(w_up.shape, BF16),
            pltpu.VMEM(w_down.shape, BF16),
            pltpu.VMEM((n, rc, heads, 128), F32),
            pltpu.VMEM((rc, nq), BF16),
            pltpu.VMEM((n, rc, nq), BF16),
            pltpu.VMEM((rows, nq), F32),
            pltpu.VMEM((t, rows, dl), BF16),
            pltpu.VMEM((t, rows, dl), BF16),
            pltpu.VMEM((n, rows, ffc), BF16),
            pltpu.VMEM((n, rows, ffc), BF16),
            pltpu.VMEM((8, rows), F32),
            pltpu.VMEM((n, 8, rows), F32),
            pltpu.VMEM((n, rows, ffc), BF16),
            dma((3,)), dma((10, n)), dma((4, t)),
        ],
        compiler_params=pltpu.CompilerParams(collective_id=1, has_side_effects=True),
    )(packed, own, tokens, mlp_gain[None, :], w_out, w_up, w_down)


def solution(mesh):
    in_specs = (
        P(None, "kv"),
        P("kv"),
        P("kv", "tp"),
        P("kv", "tp"),
        P("kv", "tp"),
        P("kv", "tp"),
        P(),
        P(None, "tp", None, "kv"),
        P(None, "tp", None, "kv"),
        P(None, "tp", "kv"),
        P("tp", "kv"),
        P("kv"),
        P("kv", "tp"),
        P("tp", "kv"),
    )
    body = functools.partial(shards, mesh.shape["kv"], mesh.shape["tp"])
    return jax.shard_map(
        body, mesh=mesh, in_specs=in_specs, out_specs=P(None, "kv"), check_vma=False
    )
```

```python
import functools

import jax
import jax.numpy as jnp
from jax import lax
from jax.experimental import pallas as pl
from jax.experimental.pallas import tpu as pltpu
from jax.sharding import PartitionSpec as P

MESH = pl.DeviceIdType.MESH
HEAD_DIM = 64
EPS = 1e-06
F32 = jnp.float32
BF16 = jnp.bfloat16


def greet(n, t, with_tp):
    kv, tp = lax.axis_index("kv"), lax.axis_index("tp")
    barrier = pltpu.get_barrier_semaphore()
    count = n - 1
    for i in range(1, n):
        pl.semaphore_signal(
            barrier, inc=1, device_id=(lax.rem(kv + i, n), tp), device_id_type=MESH
        )
    if with_tp:
        count += t - 1
        for i in range(1, t):
            pl.semaphore_signal(
                barrier, inc=1, device_id=(kv, lax.rem(tp + i, t)), device_id_type=MESH
            )
    pl.semaphore_wait(barrier, count)


def remote(src, dst, send, recv, kv, tp):
    return pltpu.make_async_remote_copy(
        src_ref=src,
        dst_ref=dst,
        send_sem=send,
        recv_sem=recv,
        device_id=(kv, tp),
        device_id_type=MESH,
    )


def project_kernel(
    n, t, d, tok, gain, wq, wk, wv, wf, qgain, out, parts, got, mine, ssem, rsem, asem, bsem
):
    kv, tp = lax.axis_index("kv"), lax.axis_index("tp")
    greet(n, t, False)
    rows = tok.shape[0]
    rc = rows // n
    nq, nk, nf = wq.shape[1], wk.shape[1], wf.shape[0]
    stream = tok[...].astype(F32)
    squares = jnp.sum(stream * stream, axis=1, keepdims=True)
    normed = (stream * gain[...]).astype(BF16)
    q = jnp.dot(normed, wq[...], preferred_element_type=F32)
    k = jnp.dot(normed, wk[...], preferred_element_type=F32)
    v = jnp.dot(normed, wv[...], preferred_element_type=F32)
    f = lax.dot_general(
        normed, wf[...], (((1,), (1,)), ((), ())), preferred_element_type=F32
    )
    for p in range(n):
        cut = slice(p * rc, (p + 1) * rc)
        parts[p, :, 0:nq] = q[cut]
        parts[p, :, nq : nq + nk] = k[cut]
        parts[p, :, nq + nk : nq + 2 * nk] = v[cut]
        base = nq + 2 * nk
        parts[p, :, base : base + 128] = jnp.broadcast_to(squares[cut], (rc, 128))
        parts[p, :, base : base + nf] = f[cut]
    sends = []
    for i in range(1, n):
        peer = lax.rem(kv + i, n)
        c = remote(parts.at[peer], got.at[i], ssem.at[i], rsem.at[i], peer, tp)
        c.start()
        sends.append(c)
    total = parts[kv]
    for c in sends:
        c.wait_recv()
    for i in range(1, n):
        total = total + got[i]
    base = nq + 2 * nk
    scale = lax.rsqrt(total[:, base + 127 : base + 128] / d + EPS)
    scaled = total * scale
    raw = scaled[:, 0:nq]
    raw2 = raw * raw
    head = lax.broadcasted_iota(jnp.int32, raw.shape, 1) // HEAD_DIM
    inverse = jnp.zeros_like(raw)
    for h in range(nq // HEAD_DIM):
        on = head == h
        mean = jnp.sum(jnp.where(on, raw2, 0.0), axis=1, keepdims=True) / HEAD_DIM
        inverse = jnp.where(on, lax.rsqrt(mean + EPS), inverse)
    gains = jnp.concatenate([qgain[...]] * (nq // HEAD_DIM), axis=1)
    mine[:, 0:nq] = raw * inverse * gains
    mine[:, nq:base] = scaled[:, nq:base]
    gate = scaled[:, base:]
    mine[:, base:] = jnp.minimum(gate, 0.0) - jnp.log1p(jnp.exp(-jnp.abs(gate)))
    gathers = []
    for i in range(1, n):
        peer = lax.rem(kv + i, n)
        c = remote(mine, out.at[kv], asem.at[i], bsem.at[i], peer, tp)
        c.start()
        gathers.append(c)
    out[kv] = mine[...]
    for i in range(1, n):
        gathers[i - 1].wait_recv()
    for c in sends + gathers:
        c.wait_send()


def attend_kernel(sharing, q_ref, k_ref, v_ref, d_ref, o_ref):
    steps, heads, _ = q_ref.shape
    groups = heads // sharing
    row = lax.broadcasted_iota(jnp.int32, (heads, HEAD_DIM), 0) // sharing
    scores = [
        jnp.dot(q_ref[i], k_ref[i], preferred_element_type=F32) * (HEAD_DIM**-0.5) + d_ref[i]
        for i in range(steps)
    ]
    peaks = [jnp.max(s, axis=1, keepdims=True) for s in scores]
    weights = [jnp.exp(s - m) for s, m in zip(scores, peaks)]
    sums = [jnp.sum(w, axis=1, keepdims=True) for w in weights]
    outs = [
        lax.dot_general(
            w.astype(BF16), v_ref[i], (((1,), (1,)), ((), ())), preferred_element_type=F32
        )
        for i, w in enumerate(weights)
    ]
    for i in range(steps):
        o = outs[i]
        picked = o[:, 0:HEAD_DIM]
        for g in range(1, groups):
            picked = jnp.where(row == g, o[:, g * HEAD_DIM : (g + 1) * HEAD_DIM], picked)
        o_ref[i, :, 0:64] = picked
        o_ref[i, :, 64:96] = jnp.broadcast_to(peaks[i], (heads, 32))
        o_ref[i, :, 96:128] = jnp.broadcast_to(sums[i], (heads, 32))


def rest_kernel(
    n, t, d, packed, own, tok, gain, wo_hbm, wu_hbm, wd_hbm, out,
    wo, wu, wd, got, att, allatt, full, tpa, tpb, upsend, upgot, upsend2, upgot2, keep, sqs, sqgot, hid,
    wsem, sem, tsem,
):
    kv, tp = lax.axis_index("kv"), lax.axis_index("tp")
    loads = [
        pltpu.make_async_copy(a, b, wsem.at[j])
        for j, (a, b) in enumerate(((wo_hbm, wo), (wu_hbm, wu), (wd_hbm, wd)))
    ]
    for c in loads:
        c.start()
    greet(n, t, True)
    rows, heads, _ = packed.shape
    rc = rows // n
    ffc = wu.shape[1] // n
    started = []

    def send(kind, i, src, dst, peer=None):
        if peer is None:
            peer = lax.rem(kv + i, n)
        c = remote(src(peer), dst, sem.at[2 * kind, i], sem.at[2 * kind + 1, i], peer, tp)
        c.start()
        started.append(c)
        return c

    def tp_sum(kind, buf, value):
        buf[tp] = value.astype(BF16)
        copies = []
        for i in range(1, t):
            c = remote(
                buf.at[tp], buf.at[tp], tsem.at[2 * kind, i], tsem.at[2 * kind + 1, i],
                kv, lax.rem(tp + i, t),
            )
            c.start()
            copies.append(c)
            started.append(c)
        for c in copies:
            c.wait_recv()
        total = buf[0].astype(F32)
        for j in range(1, t):
            total = total + buf[j].astype(F32)
        return total.astype(BF16).astype(F32)

    copies = [
        send(0, i, lambda p: packed.at[pl.ds(p * rc, rc)], got.at[i]) for i in range(1, n)
    ]
    mine = packed[pl.ds(kv * rc, rc)]
    extra = own[pl.ds(kv * rc, rc)]
    own_score = extra[:, :, 64:65]
    forget = extra[:, :, 96:97]
    for c in copies:
        c.wait_recv()
    blocks = [mine] + [got[i] for i in range(1, n)]
    peaks = [b[:, :, 64:65] + forget for b in blocks]
    peak = own_score
    for p in peaks:
        peak = jnp.maximum(peak, p)
    own_weight = jnp.exp(own_score - peak)
    mass = own_weight
    summed = own_weight.astype(BF16).astype(F32) * extra[:, :, 0:64]
    for b, p in zip(blocks, peaks):
        w = jnp.exp(p - peak)
        mass = mass + w * b[:, :, 96:97]
        summed = summed + w * b[:, :, 0:64]
    head = summed / mass
    for h in range(heads):
        att[:, h * HEAD_DIM : (h + 1) * HEAD_DIM] = head[:, h, :].astype(BF16)
    copies = [send(1, i, lambda p: att, allatt.at[kv]) for i in range(1, n)]
    allatt[kv] = att[...]
    loads[0].wait()
    for c in copies:
        c.wait_recv()
    for p in range(n):
        full[p * rc : (p + 1) * rc, :] = allatt[p].astype(F32)
    attn = jnp.dot(full[...].astype(BF16), wo[...], preferred_element_type=F32)
    attn = tp_sum(0, tpa, attn)
    residual = (tok[...].astype(F32) + attn).astype(BF16).astype(F32)
    normed = (residual * gain[...]).astype(BF16)
    loads[1].wait()
    half = n // 2
    side = lax.rem(kv, 2)
    place = kv // 2
    partner = kv + 1 - 2 * side
    order = list(range(1, half)) + [0]

    def term(dest):
        cols = pl.ds(pl.multiple_of(dest * ffc, ffc), ffc)
        return jnp.dot(normed, wu[:, cols], preferred_element_type=F32)

    firsts = {}
    for j in order:
        upsend[j] = term(2 * lax.rem(place + j, half) + 1 - side).astype(BF16)
        firsts[j] = send(2, j, lambda p: upsend.at[j], upgot.at[j], partner)
    for j in order:
        keep[j] = term(2 * lax.rem(place + j, half) + side)
    sqs[...] = lax.dot_general(
        jnp.ones((8, residual.shape[1]), F32),
        residual * residual,
        (((1,), (1,)), ((), ())),
        preferred_element_type=F32,
        precision=lax.Precision.HIGHEST,
    )
    sq_copies = [send(3, i, lambda p: sqs, sqgot.at[i]) for i in range(1, n)]
    seconds = {}
    for j in order:
        firsts[j].wait_recv()
        part = keep[j] + upgot[j].astype(F32)
        if j:
            upsend2[j] = part.astype(BF16)
            seconds[j] = send(
                4, j, lambda p: upsend2.at[j], upgot2.at[j], 2 * lax.rem(place + j, half) + side
            )
    total = sqs[...]
    for i in range(1, n):
        sq_copies[i - 1].wait_recv()
        total = total + sqgot[i]
    r = lax.broadcasted_iota(jnp.int32, (rows, rows), 0)
    c_ = lax.broadcasted_iota(jnp.int32, (rows, rows), 1)
    wide = jnp.broadcast_to(total[0:1, :], (rows, rows))
    column = jnp.sum(jnp.where(r == c_, wide, 0.0), axis=1, keepdims=True)
    scale = lax.rsqrt(column / d + EPS)
    for j in range(1, half):
        seconds[j].wait_recv()
        part = part + upgot2[j].astype(F32)
    hidden = jnp.square(jnp.maximum(part * scale, 0.0)).astype(BF16)
    hid[kv] = hidden
    across = {0: send(6, 0, lambda p: hid.at[kv], hid.at[kv], partner)}
    along = {}
    for j in range(1, half):
        along[j] = send(
            5, j, lambda p: hid.at[kv], hid.at[kv], 2 * lax.rem(place + j, half) + side
        )
    loads[2].wait()

    def lower(src):
        there = pl.ds(pl.multiple_of(src * ffc, ffc), ffc)
        return jnp.dot(hid[src], wd[there, :], preferred_element_type=F32)

    down = lower(kv)
    for j in range(1, half):
        src = 2 * lax.rem(place + half - j, half) + side
        along[j].wait_recv()
        across[j] = send(6, j, lambda p: hid.at[src], hid.at[src], partner)
        down = down + lower(src)
    for j in range(half):
        across[j].wait_recv()
        down = down + lower(2 * lax.rem(place + half - j, half) + 1 - side)
    mlp = tp_sum(1, tpb, down)
    out[...] = (residual + mlp).astype(BF16)
    for c in started:
        c.wait_send()


def shards(
    n, t, tokens, mix_gain, w_query, w_key, w_value, w_forget, query_gain,
    key_cache, value_cache, decay_cache, w_out, mlp_gain, w_up, w_down,
):
    rows, dl = tokens.shape
    d = dl * n
    rc = rows // n
    heads = w_forget.shape[1]
    groups = key_cache.shape[1]
    sharing = heads // groups
    nq, nk = w_query.shape[1], w_key.shape[1]
    span = key_cache.shape[3]
    vmem = pl.BlockSpec(memory_space=pltpu.VMEM)
    anywhere = pl.BlockSpec(memory_space=pl.ANY)
    nk_pad = nk
    width = nq + 2 * nk_pad + 128
    dma = pltpu.SemaphoreType.DMA
    proj = pl.pallas_call(
        functools.partial(project_kernel, n, t, d),
        out_shape=jax.ShapeDtypeStruct((n, rc, width), F32),
        in_specs=[vmem] * 7,
        out_specs=vmem,
        scratch_shapes=[
            pltpu.VMEM((n, rc, width), F32),
            pltpu.VMEM((n, rc, width), F32),
            pltpu.VMEM((rc, width), F32),
            dma((n,)), dma((n,)), dma((n,)), dma((n,)),
        ],
        compiler_params=pltpu.CompilerParams(collective_id=0, has_side_effects=True),
    )(
        tokens, mix_gain[None, :], w_query, w_key, w_value, w_forget.T, query_gain[None, :],
    ).reshape(rows, width)
    query = proj[:, :nq].astype(BF16).reshape(rows, groups, sharing, HEAD_DIM)
    key_new = proj[:, nq : nq + nk].astype(BF16).reshape(rows, groups, HEAD_DIM)
    value_new = proj[:, nq + nk : nq + 2 * nk].astype(BF16).astype(F32)
    value_new = value_new.reshape(rows, groups, 1, HEAD_DIM)
    forget = proj[:, nq + 2 * nk : nq + 2 * nk + heads].reshape(rows, heads, 1)
    own_score = jnp.sum(
        query.astype(F32) * key_new.astype(F32)[:, :, None, :], axis=-1
    ) * (HEAD_DIM**-0.5)
    own = jnp.concatenate(
        [
            jnp.broadcast_to(value_new, (rows, groups, sharing, HEAD_DIM)).reshape(
                rows, heads, HEAD_DIM
            ),
            jnp.broadcast_to(own_score.reshape(rows, heads, 1), (rows, heads, 32)),
            jnp.broadcast_to(forget, (rows, heads, 32)),
        ],
        axis=-1,
    )
    same = jnp.eye(groups, dtype=jnp.bool_)[None, :, None, :, None]
    spread = jnp.where(same, query[:, :, :, None, :], jnp.zeros((), BF16))
    spread = spread.reshape(rows, heads, groups * HEAD_DIM)
    step = 8
    block = lambda a, b: pl.BlockSpec((step, a, b), lambda i: (i, 0, 0))
    gd = groups * HEAD_DIM
    packed = pl.pallas_call(
        functools.partial(attend_kernel, sharing),
        grid=(rows // step,),
        out_shape=jax.ShapeDtypeStruct((rows, heads, 128), F32),
        in_specs=[block(heads, gd), block(gd, span), block(gd, span), block(heads, span)],
        out_specs=block(heads, 128),
    )(
        spread,
        key_cache.reshape(rows, gd, span),
        value_cache.reshape(rows, gd, span),
        decay_cache,
    )
    ff = w_up.shape[1]
    ffc = ff // n
    return pl.pallas_call(
        functools.partial(rest_kernel, n, t, d),
        out_shape=jax.ShapeDtypeStruct((rows, dl), BF16),
        in_specs=[vmem] * 4 + [anywhere] * 3,
        out_specs=vmem,
        scratch_shapes=[
            pltpu.VMEM(w_out.shape, BF16),
            pltpu.VMEM(w_up.shape, BF16),
            pltpu.VMEM(w_down.shape, BF16),
            pltpu.VMEM((n, rc, heads, 128), F32),
            pltpu.VMEM((rc, nq), BF16),
            pltpu.VMEM((n, rc, nq), BF16),
            pltpu.VMEM((rows, nq), F32),
            pltpu.VMEM((t, rows, dl), BF16),
            pltpu.VMEM((t, rows, dl), BF16),
            pltpu.VMEM((n // 2, rows, ffc), BF16),
            pltpu.VMEM((n // 2, rows, ffc), BF16),
            pltpu.VMEM((n // 2, rows, ffc), BF16),
            pltpu.VMEM((n // 2, rows, ffc), BF16),
            pltpu.VMEM((n // 2, rows, ffc), F32),
            pltpu.VMEM((8, rows), F32),
            pltpu.VMEM((n, 8, rows), F32),
            pltpu.VMEM((n, rows, ffc), BF16),
            dma((3,)), dma((14, n)), dma((4, t)),
        ],
        compiler_params=pltpu.CompilerParams(collective_id=1, has_side_effects=True),
    )(packed, own, tokens, mlp_gain[None, :], w_out, w_up, w_down)


def solution(mesh):
    in_specs = (
        P(None, "kv"),
        P("kv"),
        P("kv", "tp"),
        P("kv", "tp"),
        P("kv", "tp"),
        P("kv", "tp"),
        P(),
        P(None, "tp", None, "kv"),
        P(None, "tp", None, "kv"),
        P(None, "tp", "kv"),
        P("tp", "kv"),
        P("kv"),
        P("kv", "tp"),
        P("tp", "kv"),
    )
    body = functools.partial(shards, mesh.shape["kv"], mesh.shape["tp"])
    return jax.shard_map(
        body, mesh=mesh, in_specs=in_specs, out_specs=P(None, "kv"), check_vma=False
    )
```
